32 devices in a mesh: gr: 4 (over z), sp: 4 (over y, x), tp: 2 (over core).
Axes of the slice: x: 2, y: 2, z: 4, core: 2. Of those that a mesh axis runs over, the one named last changes fastest.
Arguments:
- prompt: bfloat16 [16, 512, 4096], P('gr', 'sp'), may hold values from -16 to 16
- forget_weight: bfloat16 [4096, 2048], P(None, 'tp'), may hold values from -0.09375 to 0.09375
- value_weight: bfloat16 [4096, 2048], P(None, 'tp'), may hold values from -0.09375 to 0.09375
- leak: float32 [2048], P('tp'), may hold values from 0 to 1, as said below
- query: bfloat16 [16, 2048], P('gr', 'tp'), may hold values from -6 to 6
- next_input: bfloat16 [16, 4096], P('gr'), may hold values from -6 to 6
- read_gain: float32 [2048], P('tp'), may hold values from 0.1 to 1.9
Outputs:
- state_cache: bfloat16 [16, 16, 128, 128], P('gr', 'tp', 'sp')
- read_out: bfloat16 [16, 2048], P('gr', 'tp')
The draws below stay inside these ranges and needn't reach their ends.
Inputs may be any that keep to these rules, and one draw needn't show every extreme that they name: `leak`: positive, at most one half.
All inputs are finite; a program needn't handle non-finite values.
Results may differ from the reference program's by a relative error of at most 0.0062.
Values sent between devices are 32-bit elements; how exact they have to be, the bound alone decides.
A program may use at most 64 MiB of HBM per device.

```python
import jax
import jax.numpy as jnp
from jax import lax

D = 4096
HEADS = 16
DK = 128
DV = 128
POS_DEV = 128
SEQS = 16
LEN = 512
N_SP = 4


def draw_prompt(key, part):
    key_scale = jax.random.fold_in(key, 11)
    key_main = jax.random.fold_in(key, 12)
    blocks = LEN // 8
    log_scale = jax.random.uniform(key_scale, (SEQS, blocks, 1), jnp.float32, jnp.log(0.4), jnp.log(2.5))
    scale = jnp.repeat(jnp.exp(log_scale), 8, axis=1)
    values = jax.random.normal(key_main, (SEQS, LEN, D), jnp.float32) * scale
    return jnp.clip(values, -16.0, 16.0).astype(jnp.bfloat16)


def draw_leak(key, part):
    key_main = jax.random.fold_in(key, 21)
    length = float(LEN)
    low = 0.4 / length
    high = min(120.0 / length, 0.5)
    spread = jax.random.uniform(key_main, (HEADS * DK,), jnp.float32)
    return jnp.exp(jnp.log(low) + spread * (jnp.log(high) - jnp.log(low))).astype(jnp.float32)


def steps_of(rng, extent, pieces, smallest, largest):
    def one(axis_at, parts):
        steps = jax.random.uniform(jax.random.fold_in(jax.random.fold_in(rng, 6), axis_at), (parts,), jnp.float32, smallest / len(pieces), largest / len(pieces))
        return jnp.repeat(jnp.exp(steps), extent[axis_at] // parts).reshape((-1,) + (1,) * (len(extent) - axis_at - 1))

    level = one(*pieces[0])
    for cut in pieces[1:]:
        level = level * one(*cut)
    return level


def normal_values(key, shape, width, most, split=(), dtype=jnp.bfloat16):
    drawn = width * jax.random.normal(key, shape, jnp.float32)
    if split:
        drawn = drawn * steps_of(key, shape, split, -0.22, 0.18)
    return jnp.clip(drawn, -most, most).astype(dtype)


def setup_inputs(seed: int = 0) -> dict:
    arg_keys = jax.random.split(jax.random.key(seed), 8)
    return {
        "prompt": draw_prompt(jax.random.fold_in(arg_keys[7], 71), 0),
        "forget_weight": normal_values(arg_keys[1], (D, HEADS * DK), D ** -0.5, 0.09375, ((1, 2),)),
        "value_weight": normal_values(arg_keys[2], (D, HEADS * DV), D ** -0.5, 0.09375, ((1, 2),)),
        "leak": draw_leak(jax.random.fold_in(arg_keys[7], 71), 0),
        "query": normal_values(arg_keys[4], (SEQS, HEADS * DK), 1.0, 6.0, ((0, 4), (1, 2))),
        "next_input": normal_values(arg_keys[5], (SEQS, D), 1.0, 6.0, ((0, 4),)),
        "read_gain": jnp.clip(1.0 + 0.18 * jax.random.normal(arg_keys[6], (HEADS * DV,), jnp.float32), 0.1, 1.9),
    }


def sequence_state(seq_rows, forget_weight, value_weight, leak):
    gate_pre = jnp.dot(seq_rows, forget_weight, preferred_element_type=jnp.float32)
    values = jnp.dot(seq_rows, value_weight, preferred_element_type=jnp.float32).astype(jnp.bfloat16)
    inflow = leak * jax.nn.sigmoid(-gate_pre)
    decay_log = jnp.log1p(-inflow)
    inflow = inflow.reshape(N_SP, POS_DEV, HEADS, DK)
    decay_log = decay_log.reshape(N_SP, POS_DEV, HEADS, DK)
    values = values.reshape(N_SP, POS_DEV, HEADS, DV)
    seg_cum = jnp.cumsum(decay_log, axis=1)
    seg_total = seg_cum[:, -1]
    weighted = (inflow * jnp.exp(seg_total[:, None] - seg_cum)).astype(jnp.bfloat16)
    seg_state = jnp.einsum('nphk,nphv->nhkv', weighted.astype(jnp.float32), values.astype(jnp.float32))
    later = jnp.cumsum(seg_total[::-1], axis=0)[::-1] - seg_total
    return lax.optimization_barrier(jnp.sum(jnp.exp(later)[..., None] * seg_state, axis=0))

def reference(prompt, forget_weight, value_weight, leak, query, next_input, read_gain):
    states = lax.map(lambda rows: sequence_state(rows, forget_weight, value_weight, leak), prompt)
    next_pre = jnp.dot(next_input, forget_weight, preferred_element_type=jnp.float32).reshape(SEQS, HEADS, DK)
    next_values = jnp.dot(next_input, value_weight, preferred_element_type=jnp.float32).astype(jnp.bfloat16)
    next_values = next_values.astype(jnp.float32).reshape(SEQS, HEADS, DV)
    next_inflow = leak.reshape(HEADS, DK) * jax.nn.sigmoid(-next_pre)
    next_forget = 1.0 - next_inflow
    read_state = next_forget[..., None] * states + next_inflow[..., None] * next_values[:, :, None, :]
    queries = query.astype(jnp.float32).reshape(SEQS, HEADS, DK)
    raw_read = lax.optimization_barrier(jnp.sum(queries[..., None] * read_state, axis=2))
    scaled = raw_read * lax.rsqrt(lax.optimization_barrier(jnp.mean(raw_read * raw_read, axis=-1, keepdims=True)) + 1e-06)
    read_out = (scaled * read_gain.reshape(HEADS, DV)).astype(jnp.bfloat16).reshape(SEQS, HEADS * DV)
    return (states.astype(jnp.bfloat16), read_out)
```

```python
import functools

import jax
import jax.numpy as jnp
from jax import lax
from jax.experimental import pallas as pl
from jax.experimental.pallas import tpu as pltpu
from jax.sharding import PartitionSpec as P

DK = 128
DV = 128
PAIR = 2
PAD = 16
F32 = jnp.float32
BF16 = jnp.bfloat16


def suffix_product(x):
    rows = x.shape[0]
    step = 1
    while step < rows:
        x = x * jnp.concatenate([x[step:], jnp.ones((step, x.shape[1]), F32)], axis=0)
        step *= 2
    return x


def kernel(
    seqs, span, chunks,
    prompt, forget_w, value_w, leak, query, nxt, gain,
    cache, read_out,
    x_v, fw_v, vw_v, pad_v, gate_v, val_v, keys_v, qf_v, qi_v, nv_v,
    totals, states, stage1, stage2, reads,
    load_sem, tot_s, tot_r, s1_s, s1_r, s2_s, s2_r, rd_s, rd_r,
):
    me = lax.axis_index("sp")
    count = 4
    xbit, ybit = me % 2, me // 2
    xpeer = me + 1 - 2 * xbit
    ypeer = me + 2 - 4 * ybit
    dpeer = 3 - me
    peers = (xpeer, ypeer, dpeer)
    rows = seqs * span
    wide = PAIR * DK
    kdev = DK // count

    def cols(c):
        return slice(c * wide, (c + 1) * wide)

    def load_w(c, which):
        src, dst = ((forget_w, fw_v), (value_w, vw_v))[which]
        return pltpu.make_async_copy(
            src.at[:, cols(c)], dst.at[:, cols(c)], load_sem.at[1 + 2 * c + which]
        )

    load_x = pltpu.make_async_copy(prompt, x_v.at[pl.ds(0, rows)], load_sem.at[0])
    load_x.start()
    load_w(0, 0).start()
    for c in range(chunks):
        if c + 1 < chunks:
            load_w(c + 1, 0).start()
        load_w(c, 1).start()

    barrier = pltpu.get_barrier_semaphore()
    for peer in peers:
        pl.semaphore_signal(barrier, inc=1, device_id={"sp": peer})
    pad_v[...] = jnp.zeros_like(pad_v)
    pad_v[0:seqs, :] = nxt[...].astype(F32)
    x_v[rows:, :] = pad_v[...].astype(BF16)
    pl.semaphore_wait(barrier, 3)

    def tot_copy(c, i):
        return pltpu.make_async_remote_copy(
            src_ref=totals.at[c, me], dst_ref=totals.at[c, me],
            send_sem=tot_s.at[c, i], recv_sem=tot_r.at[c, i],
            device_id={"sp": peers[i]},
        )

    def read_copy(i):
        return pltpu.make_async_remote_copy(
            src_ref=reads.at[me], dst_ref=reads.at[me],
            send_sem=rd_s.at[i], recv_sem=rd_r.at[i],
            device_id={"sp": peers[i]},
        )

    def s1_copy(c, j):
        bit, peer = ((xbit, xpeer), (ybit, ypeer))[j]
        return pltpu.make_async_remote_copy(
            src_ref=states.at[c, j, 1 - bit], dst_ref=stage1.at[c, j],
            send_sem=s1_s.at[c, j], recv_sem=s1_r.at[c, j],
            device_id={"sp": peer},
        )

    def s2_copy(c, j):
        bit, (bit2, peer) = ((xbit, (ybit, ypeer)), (ybit, (xbit, xpeer)))[j]
        return pltpu.make_async_remote_copy(
            src_ref=states.at[c, j, bit, 1 - bit2], dst_ref=stage2.at[c, j],
            send_sem=s2_s.at[c, j], recv_sem=s2_r.at[c, j],
            device_id={"sp": peer},
        )

    def gates(c):
        load_w(c, 0).wait()
        gate_v[...] = jnp.dot(x_v[...], fw_v[:, cols(c)], preferred_element_type=F32)
        lk = leak[:, cols(c)]
        for s in range(seqs):
            at = slice(s * span, (s + 1) * span)
            inflow = lk * jax.nn.sigmoid(-gate_v[at, :])
            forget = 1.0 - inflow
            after = suffix_product(
                jnp.concatenate([forget[1:], jnp.ones((1, wide), F32)], axis=0)
            )
            keys_v[c % 2, at, :] = inflow * after
            totals[c, me, s : s + 1, :] = forget[0:1] * after[0:1]
        n_in = lk * jax.nn.sigmoid(-gate_v[rows : rows + seqs, :])
        q = query[:, cols(c)].astype(F32)
        qf_v[:, cols(c)] = q * (1.0 - n_in)
        qi_v[:, cols(c)] = q * n_in
        for i in range(3):
            tot_copy(c, i).start()

    def segment_states(c):
        load_w(c, 1).wait()
        val_v[...] = jnp.dot(x_v[...], vw_v[:, cols(c)], preferred_element_type=F32).astype(BF16)
        nv_v[:, cols(c)] = val_v[rows:, :].astype(F32)
        for i in range(3):
            tot_copy(c, i).wait_recv()
        later = jnp.ones((seqs, wide), F32)
        for source in range(1, count):
            part = totals[c, source, 0:seqs, :]
            later = later * jnp.where(source > me, part, jnp.ones_like(part))
        for s in range(seqs):
            at = slice(s * span, (s + 1) * span)
            weighted = (keys_v[c % 2, at, :] * later[s : s + 1]).astype(BF16)
            weighed = weighted.astype(F32) * qf_v[s : s + 1, cols(c)]
            for j in range(PAIR):
                head = slice(j * DK, (j + 1) * DK)
                v = val_v[at, head]
                state = lax.dot_general(
                    weighted[:, head], v, (((0,), (0,)), ((), ())),
                    preferred_element_type=F32,
                )
                for owner in range(count):
                    first, second = (owner % 2, owner // 2)[:: 1 if j == 0 else -1]
                    states[c, j, first, second, s * kdev : (s + 1) * kdev, :] = state[
                        owner * kdev : (owner + 1) * kdev
                    ]
                a = jnp.sum(weighed[:, head], axis=1, keepdims=True)
                reads[me, s : s + 1, c * wide + j * DV : c * wide + (j + 1) * DV] = jnp.sum(
                    a * v.astype(F32), axis=0, keepdims=True
                )
        for j in range(PAIR):
            s1_copy(c, j).start()

    def combine(c):
        for j in range(PAIR):
            bit = (xbit, ybit)[j]
            s1_copy(c, j).wait_recv()
            states[c, j, bit] = states[c, j, bit] + stage1[c, j]
            s2_copy(c, j).start()

    def finish(c):
        for j in range(PAIR):
            bit, bit2 = ((xbit, ybit), (ybit, xbit))[j]
            s2_copy(c, j).wait_recv()
            owned = states[c, j, bit, bit2] + stage2[c, j]
            for s in range(seqs):
                cache[s, c * PAIR + j] = owned[s * kdev : (s + 1) * kdev].astype(BF16)

    load_x.wait()
    gates(0)
    for c in range(chunks):
        if c + 1 < chunks:
            gates(c + 1)
        segment_states(c)
        if c + 1 == chunks:
            for i in range(3):
                read_copy(i).start()
        if c >= 1:
            combine(c - 1)
        if c >= 2:
            finish(c - 2)
    combine(chunks - 1)
    for i in range(3):
        read_copy(i).wait_recv()
    raw = reads[0]
    for source in range(1, count):
        raw = raw + reads[source]
    for h in range(chunks * PAIR):
        head = slice(h * DV, (h + 1) * DV)
        inner = jnp.sum(qi_v[:, head], axis=1, keepdims=True)
        r = raw[0:seqs, head] + inner * nv_v[0:seqs, head]
        scale = lax.rsqrt(jnp.mean(r * r, axis=1, keepdims=True) + 1e-06)
        read_out[:, head] = (r * scale * gain[:, head]).astype(BF16)
    for c in range(max(chunks - 2, 0), chunks):
        finish(c)
    for c in range(chunks):
        for i in range(3):
            tot_copy(c, i).wait_send()
        for j in range(PAIR):
            s1_copy(c, j).wait_send()
            s2_copy(c, j).wait_send()
    for i in range(3):
        read_copy(i).wait_send()


def fused(prompt, forget_weight, value_weight, leak, query, next_input, read_gain):
    seqs, span, width = prompt.shape
    here = forget_weight.shape[1]
    heads = here // DK
    chunks = heads // PAIR
    wide = PAIR * DK
    count = lax.axis_size("sp")
    kdev = DK // count
    rows = seqs * span
    srows = -(-seqs // 8) * 8
    anyspace = pl.BlockSpec(memory_space=pl.ANY)
    vm = pl.BlockSpec(memory_space=pltpu.VMEM)
    dma = pltpu.SemaphoreType.DMA
    return pl.pallas_call(
        functools.partial(kernel, seqs, span, chunks),
        out_shape=(
            jax.ShapeDtypeStruct((seqs, heads, kdev, DV), BF16),
            jax.ShapeDtypeStruct((seqs, here), BF16),
        ),
        in_specs=[anyspace, anyspace, anyspace, vm, vm, vm, vm],
        out_specs=(vm, vm),
        scratch_shapes=[
            pltpu.VMEM((rows + PAD, width), BF16),
            pltpu.VMEM((width, here), BF16),
            pltpu.VMEM((width, here), BF16),
            pltpu.VMEM((PAD, width), F32),
            pltpu.VMEM((rows + PAD, wide), F32),
            pltpu.VMEM((rows + PAD, wide), BF16),
            pltpu.VMEM((2, rows, wide), F32),
            pltpu.VMEM((seqs, here), F32),
            pltpu.VMEM((seqs, here), F32),
            pltpu.VMEM((PAD, here), F32),
            pltpu.VMEM((chunks, count, srows, wide), F32),
            pltpu.VMEM((chunks, PAIR, 2, 2, seqs * kdev, DV), F32),
            pltpu.VMEM((chunks, PAIR, 2, seqs * kdev, DV), F32),
            pltpu.VMEM((chunks, PAIR, seqs * kdev, DV), F32),
            pltpu.VMEM((count, srows, here), F32),
            dma((1 + 2 * chunks,)),
            dma((chunks, 3)),
            dma((chunks, 3)),
            dma((chunks, PAIR)),
            dma((chunks, PAIR)),
            dma((chunks, PAIR)),
            dma((chunks, PAIR)),
            dma((3,)),
            dma((3,)),
        ],
        compiler_params=pltpu.CompilerParams(
            collective_id=0, has_side_effects=True, vmem_limit_bytes=60 * 1024 * 1024
        ),
    )(
        prompt.reshape(rows, width), forget_weight, value_weight, leak.reshape(1, here),
        query, next_input, read_gain.reshape(1, here),
    )


def prefix(part, axis, combine, identity):
    count = lax.axis_size(axis)
    place = lax.axis_index(axis)
    ahead = count - 1 - place
    gathered = lax.all_gather(part, axis)
    state = jnp.zeros_like(part) + jnp.asarray(identity, part.dtype)

    def one(step, state):
        source = count - 1 - step
        return combine(state, lax.dynamic_index_in_dim(gathered, source, 0, False))

    return lax.fori_loop(0, ahead, one, state)


def add_decay(earlier, later_part):
    return earlier + later_part


def local(prompt, forget_weight, value_weight, leak, query, next_input, read_gain):
    seqs, span, width = prompt.shape
    heads_here = forget_weight.shape[1] // DK
    flat_rows = prompt.reshape(seqs * span, width)
    gate_pre = jnp.dot(flat_rows, forget_weight, preferred_element_type=jnp.float32).reshape(
        seqs, span, heads_here, DK
    )
    values = jnp.dot(flat_rows, value_weight, preferred_element_type=jnp.float32).astype(
        jnp.bfloat16
    )
    values = values.reshape(seqs, span, heads_here, DV)
    leak_heads = leak.reshape(heads_here, DK)
    inflow = leak_heads * jax.nn.sigmoid(-gate_pre)
    seg_cum = jnp.cumsum(jnp.log1p(-inflow), axis=1)
    seg_total = seg_cum[:, -1]
    weighted = (inflow * jnp.exp(seg_total[:, None] - seg_cum)).astype(jnp.bfloat16)
    seg_state = jnp.einsum("sphk,sphv->shkv", weighted, values, preferred_element_type=jnp.float32)
    next_pre = jnp.dot(next_input, forget_weight, preferred_element_type=jnp.float32).reshape(
        seqs, heads_here, DK
    )
    next_values = jnp.dot(next_input, value_weight, preferred_element_type=jnp.float32).astype(
        jnp.bfloat16
    )
    next_values = next_values.astype(jnp.float32).reshape(seqs, heads_here, DV)
    next_inflow = leak_heads * jax.nn.sigmoid(-next_pre)
    next_forget = 1.0 - next_inflow
    queries = query.astype(jnp.float32).reshape(seqs, heads_here, DK)
    rows_here = DK // lax.axis_size("sp")
    start = lax.axis_index("sp") * rows_here
    later = prefix(seg_total, "sp", add_decay, jnp.zeros_like(seg_total))
    term = jnp.exp(later)[..., None] * seg_state
    owned = lax.psum_scatter(term, "sp", scatter_dimension=2, tiled=True)
    forget_rows = lax.dynamic_slice_in_dim(next_forget, start, rows_here, 2)
    inflow_rows = lax.dynamic_slice_in_dim(next_inflow, start, rows_here, 2)
    query_rows = lax.dynamic_slice_in_dim(queries, start, rows_here, 2)
    read_rows = forget_rows[..., None] * owned + inflow_rows[..., None] * next_values[:, :, None, :]
    partial_read = jnp.sum(query_rows[..., None] * read_rows, axis=2)
    raw_read = lax.psum(partial_read, "sp")
    cache = owned.astype(jnp.bfloat16)
    scaled = raw_read * lax.rsqrt(jnp.mean(raw_read * raw_read, axis=-1, keepdims=True) + 1e-06)
    read_out = (
        (scaled * read_gain.reshape(heads_here, DV))
        .astype(jnp.bfloat16)
        .reshape(seqs, heads_here * DV)
    )
    return (cache, read_out)


def solution(mesh):
    placed = (
        P("gr", "sp", None),
        P(None, "tp"),
        P(None, "tp"),
        P("tp"),
        P("gr", "tp"),
        P("gr", None),
        P("tp"),
    )
    return jax.shard_map(
        fused if mesh.shape["sp"] == 4 else local,
        mesh=mesh,
        in_specs=placed,
        out_specs=(P("gr", "tp", "sp", None), P("gr", "tp")),
        check_vma=False,
    )
```

```python
import functools

import jax
import jax.numpy as jnp
from jax import lax
from jax.experimental import pallas as pl
from jax.experimental.pallas import tpu as pltpu
from jax.sharding import PartitionSpec as P

DK = 128
DV = 128
PAIR = 2
PAD = 16
F32 = jnp.float32
BF16 = jnp.bfloat16


def suffix_product(x):
    rows = x.shape[0]
    step = 1
    while step < rows:
        x = x * jnp.concatenate([x[step:], jnp.ones((step, x.shape[1]), F32)], axis=0)
        step *= 2
    return x


def kernel(
    seqs, span, chunks,
    prompt, forget_w, value_w, leak, query, nxt, gain,
    cache, read_out,
    x_v, fw_v, vw_v, pad_v, gate_v, val_v, keys_v, qf_v, qi_v, nv_v,
    totals, states, stage1, stage2, reads,
    load_sem, tot_s, tot_r, s1_s, s1_r, s2_s, s2_r, rd_s, rd_r,
):
    me = lax.axis_index("sp")
    count = 4
    xbit, ybit = me % 2, me // 2
    xpeer = me + 1 - 2 * xbit
    ypeer = me + 2 - 4 * ybit
    dpeer = 3 - me
    peers = (xpeer, ypeer, dpeer)
    rows = seqs * span
    wide = PAIR * DK
    kdev = DK // count

    def cols(c):
        return pl.ds(pl.multiple_of(c * wide, wide), wide)

    def load_w(c, which):
        src, dst = ((forget_w, fw_v), (value_w, vw_v))[which]
        return pltpu.make_async_copy(
            src.at[:, cols(c)], dst.at[:, cols(c)], load_sem.at[1 + 2 * c + which]
        )

    load_x = pltpu.make_async_copy(prompt, x_v.at[pl.ds(0, rows)], load_sem.at[0])
    load_x.start()
    load_w(0, 0).start()
    for c in range(chunks):
        if c + 1 < chunks:
            load_w(c + 1, 0).start()
        load_w(c, 1).start()

    barrier = pltpu.get_barrier_semaphore()
    for peer in peers:
        pl.semaphore_signal(barrier, inc=1, device_id={"sp": peer})
    pad_v[...] = jnp.zeros_like(pad_v)
    pad_v[0:seqs, :] = nxt[...].astype(F32)
    x_v[rows:, :] = pad_v[...].astype(BF16)
    pl.semaphore_wait(barrier, 3)

    def tot_copy(c, i):
        return pltpu.make_async_remote_copy(
            src_ref=totals.at[c, me], dst_ref=totals.at[c, me],
            send_sem=tot_s.at[c, i], recv_sem=tot_r.at[c, i],
            device_id={"sp": peers[i]},
        )

    def read_copy(i):
        return pltpu.make_async_remote_copy(
            src_ref=reads.at[me], dst_ref=reads.at[me],
            send_sem=rd_s.at[i], recv_sem=rd_r.at[i],
            device_id={"sp": peers[i]},
        )

    def s1_copy(c, j):
        bit, peer = ((xbit, xpeer), (ybit, ypeer))[j]
        return pltpu.make_async_remote_copy(
            src_ref=states.at[c, j, 1 - bit], dst_ref=stage1.at[c, j],
            send_sem=s1_s.at[c, j], recv_sem=s1_r.at[c, j],
            device_id={"sp": peer},
        )

    def s2_copy(c, j):
        bit, (bit2, peer) = ((xbit, (ybit, ypeer)), (ybit, (xbit, xpeer)))[j]
        return pltpu.make_async_remote_copy(
            src_ref=states.at[c, j, bit, 1 - bit2], dst_ref=stage2.at[c, j],
            send_sem=s2_s.at[c, j], recv_sem=s2_r.at[c, j],
            device_id={"sp": peer},
        )

    def gates(c):
        load_w(c, 0).wait()
        gate_v[...] = jnp.dot(x_v[...], fw_v[:, cols(c)], preferred_element_type=F32)
        lk = leak[:, cols(c)]
        for s in range(seqs):
            at = slice(s * span, (s + 1) * span)
            inflow = lk * jax.nn.sigmoid(-gate_v[at, :])
            forget = 1.0 - inflow
            after = suffix_product(
                jnp.concatenate([forget[1:], jnp.ones((1, wide), F32)], axis=0)
            )
            keys_v[c % 2, at, :] = inflow * after
            totals[c, me, s : s + 1, :] = forget[0:1] * after[0:1]
        n_in = lk * jax.nn.sigmoid(-gate_v[rows : rows + seqs, :])
        q = query[:, cols(c)].astype(F32)
        qf_v[:, cols(c)] = q * (1.0 - n_in)
        qi_v[:, cols(c)] = q * n_in
        for i in range(3):
            tot_copy(c, i).start()

    def segment_states(c):
        load_w(c, 1).wait()
        val_v[...] = jnp.dot(x_v[...], vw_v[:, cols(c)], preferred_element_type=F32).astype(BF16)
        nv_v[:, cols(c)] = val_v[rows:, :].astype(F32)
        for i in range(3):
            tot_copy(c, i).wait_recv()
        later = jnp.ones((seqs, wide), F32)
        for source in range(1, count):
            part = totals[c, source, 0:seqs, :]
            later = later * jnp.where(source > me, part, jnp.ones_like(part))
        for s in range(seqs):
            at = slice(s * span, (s + 1) * span)
            weighted = (keys_v[c % 2, at, :] * later[s : s + 1]).astype(BF16)
            weighed = weighted.astype(F32) * qf_v[s : s + 1, cols(c)]
            for j in range(PAIR):
                head = slice(j * DK, (j + 1) * DK)
                v = val_v[at, head]
                state = lax.dot_general(
                    weighted[:, head], v, (((0,), (0,)), ((), ())),
                    preferred_element_type=F32,
                )
                for owner in range(count):
                    first, second = (owner % 2, owner // 2)[:: 1 if j == 0 else -1]
                    states[c, j, first, second, s * kdev : (s + 1) * kdev, :] = state[
                        owner * kdev : (owner + 1) * kdev
                    ]
                a = jnp.sum(weighed[:, head], axis=1, keepdims=True)
                reads[me, s : s + 1, pl.ds(pl.multiple_of(c * wide + j * DV, DV), DV)] = jnp.sum(
                    a * v.astype(F32), axis=0, keepdims=True
                )
        for j in range(PAIR):
            s1_copy(c, j).start()

    def combine(c):
        for j in range(PAIR):
            bit = (xbit, ybit)[j]
            s1_copy(c, j).wait_recv()
            states[c, j, bit] = states[c, j, bit] + stage1[c, j]
            s2_copy(c, j).start()

    def finish(c):
        for j in range(PAIR):
            bit, bit2 = ((xbit, ybit), (ybit, xbit))[j]
            s2_copy(c, j).wait_recv()
            owned = states[c, j, bit, bit2] + stage2[c, j]
            for s in range(seqs):
                cache[s, c * PAIR + j] = owned[s * kdev : (s + 1) * kdev].astype(BF16)

    load_x.wait()

    def stage(i, carry):
        @pl.when(i < chunks)
        def _():
            gates(i)

        @pl.when((i >= 1) & (i <= chunks))
        def _():
            segment_states(i - 1)

        @pl.when(i == chunks)
        def _():
            for p in range(3):
                read_copy(p).start()

        @pl.when((i >= 2) & (i <= chunks + 1))
        def _():
            combine(i - 2)

        @pl.when(i >= 3)
        def _():
            finish(i - 3)

        return carry

    lax.fori_loop(0, chunks + 2, stage, 0)
    for i in range(3):
        read_copy(i).wait_recv()
    raw = reads[0]
    for source in range(1, count):
        raw = raw + reads[source]
    for h in range(chunks * PAIR):
        head = slice(h * DV, (h + 1) * DV)
        inner = jnp.sum(qi_v[:, head], axis=1, keepdims=True)
        r = raw[0:seqs, head] + inner * nv_v[0:seqs, head]
        scale = lax.rsqrt(jnp.mean(r * r, axis=1, keepdims=True) + 1e-06)
        read_out[:, head] = (r * scale * gain[:, head]).astype(BF16)
    finish(chunks - 1)
    for c in range(chunks):
        for i in range(3):
            tot_copy(c, i).wait_send()
        for j in range(PAIR):
            s1_copy(c, j).wait_send()
            s2_copy(c, j).wait_send()
    for i in range(3):
        read_copy(i).wait_send()


def fused(prompt, forget_weight, value_weight, leak, query, next_input, read_gain):
    seqs, span, width = prompt.shape
    here = forget_weight.shape[1]
    heads = here // DK
    chunks = heads // PAIR
    wide = PAIR * DK
    count = lax.axis_size("sp")
    kdev = DK // count
    rows = seqs * span
    srows = -(-seqs // 8) * 8
    anyspace = pl.BlockSpec(memory_space=pl.ANY)
    vm = pl.BlockSpec(memory_space=pltpu.VMEM)
    dma = pltpu.SemaphoreType.DMA
    return pl.pallas_call(
        functools.partial(kernel, seqs, span, chunks),
        out_shape=(
            jax.ShapeDtypeStruct((seqs, heads, kdev, DV), BF16),
            jax.ShapeDtypeStruct((seqs, here), BF16),
        ),
        in_specs=[anyspace, anyspace, anyspace, vm, vm, vm, vm],
        out_specs=(vm, vm),
        scratch_shapes=[
            pltpu.VMEM((rows + PAD, width), BF16),
            pltpu.VMEM((width, here), BF16),
            pltpu.VMEM((width, here), BF16),
            pltpu.VMEM((PAD, width), F32),
            pltpu.VMEM((rows + PAD, wide), F32),
            pltpu.VMEM((rows + PAD, wide), BF16),
            pltpu.VMEM((2, rows, wide), F32),
            pltpu.VMEM((seqs, here), F32),
            pltpu.VMEM((seqs, here), F32),
            pltpu.VMEM((PAD, here), F32),
            pltpu.VMEM((chunks, count, srows, wide), F32),
            pltpu.VMEM((chunks, PAIR, 2, 2, seqs * kdev, DV), F32),
            pltpu.VMEM((chunks, PAIR, 2, seqs * kdev, DV), F32),
            pltpu.VMEM((chunks, PAIR, seqs * kdev, DV), F32),
            pltpu.VMEM((count, srows, here), F32),
            dma((1 + 2 * chunks,)),
            dma((chunks, 3)),
            dma((chunks, 3)),
            dma((chunks, PAIR)),
            dma((chunks, PAIR)),
            dma((chunks, PAIR)),
            dma((chunks, PAIR)),
            dma((3,)),
            dma((3,)),
        ],
        compiler_params=pltpu.CompilerParams(
            collective_id=0, has_side_effects=True, vmem_limit_bytes=60 * 1024 * 1024
        ),
    )(
        prompt.reshape(rows, width), forget_weight, value_weight, leak.reshape(1, here),
        query, next_input, read_gain.reshape(1, here),
    )


def prefix(part, axis, combine, identity):
    count = lax.axis_size(axis)
    place = lax.axis_index(axis)
    ahead = count - 1 - place
    gathered = lax.all_gather(part, axis)
    state = jnp.zeros_like(part) + jnp.asarray(identity, part.dtype)

    def one(step, state):
        source = count - 1 - step
        return combine(state, lax.dynamic_index_in_dim(gathered, source, 0, False))

    return lax.fori_loop(0, ahead, one, state)


def add_decay(earlier, later_part):
    return earlier + later_part


def local(prompt, forget_weight, value_weight, leak, query, next_input, read_gain):
    seqs, span, width = prompt.shape
    heads_here = forget_weight.shape[1] // DK
    flat_rows = prompt.reshape(seqs * span, width)
    gate_pre = jnp.dot(flat_rows, forget_weight, preferred_element_type=jnp.float32).reshape(
        seqs, span, heads_here, DK
    )
    values = jnp.dot(flat_rows, value_weight, preferred_element_type=jnp.float32).astype(
        jnp.bfloat16
    )
    values = values.reshape(seqs, span, heads_here, DV)
    leak_heads = leak.reshape(heads_here, DK)
    inflow = leak_heads * jax.nn.sigmoid(-gate_pre)
    seg_cum = jnp.cumsum(jnp.log1p(-inflow), axis=1)
    seg_total = seg_cum[:, -1]
    weighted = (inflow * jnp.exp(seg_total[:, None] - seg_cum)).astype(jnp.bfloat16)
    seg_state = jnp.einsum("sphk,sphv->shkv", weighted, values, preferred_element_type=jnp.float32)
    next_pre = jnp.dot(next_input, forget_weight, preferred_element_type=jnp.float32).reshape(
        seqs, heads_here, DK
    )
    next_values = jnp.dot(next_input, value_weight, preferred_element_type=jnp.float32).astype(
        jnp.bfloat16
    )
    next_values = next_values.astype(jnp.float32).reshape(seqs, heads_here, DV)
    next_inflow = leak_heads * jax.nn.sigmoid(-next_pre)
    next_forget = 1.0 - next_inflow
    queries = query.astype(jnp.float32).reshape(seqs, heads_here, DK)
    rows_here = DK // lax.axis_size("sp")
    start = lax.axis_index("sp") * rows_here
    later = prefix(seg_total, "sp", add_decay, jnp.zeros_like(seg_total))
    term = jnp.exp(later)[..., None] * seg_state
    owned = lax.psum_scatter(term, "sp", scatter_dimension=2, tiled=True)
    forget_rows = lax.dynamic_slice_in_dim(next_forget, start, rows_here, 2)
    inflow_rows = lax.dynamic_slice_in_dim(next_inflow, start, rows_here, 2)
    query_rows = lax.dynamic_slice_in_dim(queries, start, rows_here, 2)
    read_rows = forget_rows[..., None] * owned + inflow_rows[..., None] * next_values[:, :, None, :]
    partial_read = jnp.sum(query_rows[..., None] * read_rows, axis=2)
    raw_read = lax.psum(partial_read, "sp")
    cache = owned.astype(jnp.bfloat16)
    scaled = raw_read * lax.rsqrt(jnp.mean(raw_read * raw_read, axis=-1, keepdims=True) + 1e-06)
    read_out = (
        (scaled * read_gain.reshape(heads_here, DV))
        .astype(jnp.bfloat16)
        .reshape(seqs, heads_here * DV)
    )
    return (cache, read_out)


def solution(mesh):
    placed = (
        P("gr", "sp", None),
        P(None, "tp"),
        P(None, "tp"),
        P("tp"),
        P("gr", "tp"),
        P("gr", None),
        P("tp"),
    )
    return jax.shard_map(
        fused if mesh.shape["sp"] == 4 else local,
        mesh=mesh,
        in_specs=placed,
        out_specs=(P("gr", "tp", "sp", None), P("gr", "tp")),
        check_vma=False,
    )
```

```python
import functools

import jax
import jax.numpy as jnp
from jax import lax
from jax.experimental import pallas as pl
from jax.experimental.pallas import tpu as pltpu
from jax.sharding import PartitionSpec as P

DK = 128
DV = 128
PAIR = 2
PAD = 16
LAG = 3
F32 = jnp.float32
BF16 = jnp.bfloat16


def suffix_product(x):
    rows = x.shape[0]
    step = 1
    while step < rows:
        x = x * jnp.concatenate([x[step:], jnp.ones((step, x.shape[1]), F32)], axis=0)
        step *= 2
    return x


def kernel(
    seqs, span, chunks,
    prompt, forget_w, value_w, leak, query, nxt, gain,
    cache, read_out,
    x_v, fw_v, vw_v, pad_v, gate_v, val_v, keys_v, qf_v, qi_v, nv_v,
    totals, states, stage1, stage2, reads,
    load_sem, tot_s, tot_r, s1_s, s1_r, s2_s, s2_r, rd_s, rd_r,
):
    me = lax.axis_index("sp")
    count = 4
    xbit, ybit = me % 2, me // 2
    xpeer = me + 1 - 2 * xbit
    ypeer = me + 2 - 4 * ybit
    dpeer = 3 - me
    peers = (xpeer, ypeer, dpeer)
    rows = seqs * span
    wide = PAIR * DK
    kdev = DK // count

    def cols(c):
        return pl.ds(pl.multiple_of(c * wide, wide), wide)

    def load_w(c, which):
        src, dst = ((forget_w, fw_v), (value_w, vw_v))[which]
        return pltpu.make_async_copy(
            src.at[:, cols(c)], dst.at[:, cols(c)], load_sem.at[1 + 2 * c + which]
        )

    load_x = pltpu.make_async_copy(prompt, x_v.at[pl.ds(0, rows)], load_sem.at[0])
    load_x.start()
    load_w(0, 0).start()
    for c in range(chunks):
        if c + 1 < chunks:
            load_w(c + 1, 0).start()
        load_w(c, 1).start()

    barrier = pltpu.get_barrier_semaphore()
    for peer in peers:
        pl.semaphore_signal(barrier, inc=1, device_id={"sp": peer})
    pad_v[...] = jnp.zeros_like(pad_v)
    pad_v[0:seqs, :] = nxt[...].astype(F32)
    x_v[rows:, :] = pad_v[...].astype(BF16)
    pl.semaphore_wait(barrier, 3)

    def tot_copy(c, i):
        return pltpu.make_async_remote_copy(
            src_ref=totals.at[c, me], dst_ref=totals.at[c, me],
            send_sem=tot_s.at[c, i], recv_sem=tot_r.at[c, i],
            device_id={"sp": peers[i]},
        )

    def read_copy(c, i):
        return pltpu.make_async_remote_copy(
            src_ref=reads.at[c, me], dst_ref=reads.at[c, me],
            send_sem=rd_s.at[c, i], recv_sem=rd_r.at[c, i],
            device_id={"sp": peers[i]},
        )

    def s1_copy(c, j):
        bit, peer = ((xbit, xpeer), (ybit, ypeer))[j]
        return pltpu.make_async_remote_copy(
            src_ref=states.at[c, j, 1 - bit], dst_ref=stage1.at[c, j],
            send_sem=s1_s.at[c, j], recv_sem=s1_r.at[c, j],
            device_id={"sp": peer},
        )

    def s2_copy(c, j):
        bit, (bit2, peer) = ((xbit, (ybit, ypeer)), (ybit, (xbit, xpeer)))[j]
        return pltpu.make_async_remote_copy(
            src_ref=states.at[c, j, bit, 1 - bit2], dst_ref=stage2.at[c, j],
            send_sem=s2_s.at[c, j], recv_sem=s2_r.at[c, j],
            device_id={"sp": peer},
        )

    def gates(c):
        load_w(c, 0).wait()
        gate_v[...] = jnp.dot(x_v[...], fw_v[:, cols(c)], preferred_element_type=F32)
        lk = leak[:, cols(c)]
        for s in range(seqs):
            at = slice(s * span, (s + 1) * span)
            inflow = lk * jax.nn.sigmoid(-gate_v[at, :])
            forget = 1.0 - inflow
            after = suffix_product(
                jnp.concatenate([forget[1:], jnp.ones((1, wide), F32)], axis=0)
            )
            keys_v[c % 2, at, :] = inflow * after
            total = forget[0:1] * after[0:1]
            for j in range(PAIR):
                totals[c, me, j * seqs + s : j * seqs + s + 1, :] = total[:, j * DK : (j + 1) * DK]
        n_in = lk * jax.nn.sigmoid(-gate_v[rows : rows + seqs, :])
        q = query[:, cols(c)].astype(F32)
        qf_v[:, cols(c)] = q * (1.0 - n_in)
        qi_v[:, cols(c)] = q * n_in
        for i in range(3):
            tot_copy(c, i).start()

    def segment_states(c):
        load_w(c, 1).wait()
        val_v[...] = jnp.dot(x_v[...], vw_v[:, cols(c)], preferred_element_type=F32).astype(BF16)
        nv_v[:, cols(c)] = val_v[rows:, :].astype(F32)
        for i in range(3):
            tot_copy(c, i).wait_recv()
        later = jnp.ones((PAIR * seqs, DK), F32)
        for source in range(1, count):
            part = totals[c, source]
            later = later * jnp.where(source > me, part, jnp.ones_like(part))
        for s in range(seqs):
            at = slice(s * span, (s + 1) * span)
            to_end = jnp.concatenate(
                [later[j * seqs + s : j * seqs + s + 1] for j in range(PAIR)], axis=1
            )
            weighted = (keys_v[c % 2, at, :] * to_end).astype(BF16)
            weighed = weighted.astype(F32) * qf_v[s : s + 1, cols(c)]
            for j in range(PAIR):
                head = slice(j * DK, (j + 1) * DK)
                v = val_v[at, head]
                state = lax.dot_general(
                    weighted[:, head], v, (((0,), (0,)), ((), ())),
                    preferred_element_type=F32,
                )
                for owner in range(count):
                    first, second = (owner % 2, owner // 2)[:: 1 if j == 0 else -1]
                    states[c, j, first, second, s * kdev : (s + 1) * kdev, :] = state[
                        owner * kdev : (owner + 1) * kdev
                    ]
                a = jnp.sum(weighed[:, head], axis=1, keepdims=True)
                reads[c, me, j * seqs + s : j * seqs + s + 1, :] = jnp.sum(
                    a * v.astype(F32), axis=0, keepdims=True
                )
        for j in range(PAIR):
            s1_copy(c, j).start()
        for i in range(3):
            read_copy(c, i).start()

    def combine(c):
        for j in range(PAIR):
            bit = (xbit, ybit)[j]
            s1_copy(c, j).wait_recv()
            states[c, j, bit] = states[c, j, bit] + stage1[c, j]
            s2_copy(c, j).start()

    def finish(c):
        for j in range(PAIR):
            bit, bit2 = ((xbit, ybit), (ybit, xbit))[j]
            s2_copy(c, j).wait_recv()
            owned = states[c, j, bit, bit2] + stage2[c, j]
            for s in range(seqs):
                cache[s, c * PAIR + j] = owned[s * kdev : (s + 1) * kdev].astype(BF16)

    load_x.wait()

    def stage(i, carry):
        @pl.when(i < chunks)
        def _():
            gates(i)

        @pl.when(i >= 1)
        def _():
            segment_states(i - 1)

        @pl.when(i >= LAG)
        def _():
            combine(i - LAG)

        return carry

    lax.fori_loop(0, chunks + 1, stage, 0)
    for c in range(chunks + 1 - LAG, chunks):
        combine(c)
    for c in range(chunks - 1):
        finish(c)
    for c in range(chunks):
        for i in range(3):
            read_copy(c, i).wait_recv()
        raw = reads[c, 0]
        for source in range(1, count):
            raw = raw + reads[c, source]
        for j in range(PAIR):
            head = slice((c * PAIR + j) * DV, (c * PAIR + j + 1) * DV)
            inner = jnp.sum(qi_v[:, head], axis=1, keepdims=True)
            r = raw[j * seqs : (j + 1) * seqs] + inner * nv_v[0:seqs, head]
            scale = lax.rsqrt(jnp.mean(r * r, axis=1, keepdims=True) + 1e-06)
            read_out[:, head] = (r * scale * gain[:, head]).astype(BF16)
    finish(chunks - 1)
    for c in range(chunks):
        for i in range(3):
            tot_copy(c, i).wait_send()
        for j in range(PAIR):
            s1_copy(c, j).wait_send()
            s2_copy(c, j).wait_send()
        for i in range(3):
            read_copy(c, i).wait_send()


def hand_over(cache_in, read_in, cache, read_out):
    cache[...] = cache_in[...]
    read_out[...] = read_in[...]


def fused(prompt, forget_weight, value_weight, leak, query, next_input, read_gain):
    seqs, span, width = prompt.shape
    here = forget_weight.shape[1]
    heads = here // DK
    chunks = heads // PAIR
    wide = PAIR * DK
    count = lax.axis_size("sp")
    kdev = DK // count
    rows = seqs * span
    anyspace = pl.BlockSpec(memory_space=pl.ANY)
    vm = pl.BlockSpec(memory_space=pltpu.VMEM)
    dma = pltpu.SemaphoreType.DMA
    made = pl.pallas_call(
        functools.partial(kernel, seqs, span, chunks),
        out_shape=(
            jax.ShapeDtypeStruct((seqs, heads, kdev, DV), BF16),
            jax.ShapeDtypeStruct((seqs, here), BF16),
        ),
        in_specs=[anyspace, anyspace, anyspace, vm, vm, vm, vm],
        out_specs=(vm, vm),
        scratch_shapes=[
            pltpu.VMEM((rows + PAD, width), BF16),
            pltpu.VMEM((width, here), BF16),
            pltpu.VMEM((width, here), BF16),
            pltpu.VMEM((PAD, width), F32),
            pltpu.VMEM((rows + PAD, wide), F32),
            pltpu.VMEM((rows + PAD, wide), BF16),
            pltpu.VMEM((2, rows, wide), F32),
            pltpu.VMEM((seqs, here), F32),
            pltpu.VMEM((seqs, here), F32),
            pltpu.VMEM((PAD, here), F32),
            pltpu.VMEM((chunks, count, PAIR * seqs, DK), F32),
            pltpu.VMEM((chunks, PAIR, 2, 2, seqs * kdev, DV), F32),
            pltpu.VMEM((chunks, PAIR, 2, seqs * kdev, DV), F32),
            pltpu.VMEM((chunks, PAIR, seqs * kdev, DV), F32),
            pltpu.VMEM((chunks, count, PAIR * seqs, DV), F32),
            dma((1 + 2 * chunks,)),
            dma((chunks, 3)),
            dma((chunks, 3)),
            dma((chunks, PAIR)),
            dma((chunks, PAIR)),
            dma((chunks, PAIR)),
            dma((chunks, PAIR)),
            dma((chunks, 3)),
            dma((chunks, 3)),
        ],
        compiler_params=pltpu.CompilerParams(
            collective_id=0, has_side_effects=True, vmem_limit_bytes=60 * 1024 * 1024
        ),
    )(
        prompt.reshape(rows, width), forget_weight, value_weight, leak.reshape(1, here),
        query, next_input, read_gain.reshape(1, here),
    )
    return pl.pallas_call(
        hand_over,
        out_shape=tuple(jax.ShapeDtypeStruct(a.shape, a.dtype) for a in made),
        in_specs=[vm, vm],
        out_specs=(vm, vm),
    )(*made)


def prefix(part, axis, combine, identity):
    count = lax.axis_size(axis)
    place = lax.axis_index(axis)
    ahead = count - 1 - place
    gathered = lax.all_gather(part, axis)
    state = jnp.zeros_like(part) + jnp.asarray(identity, part.dtype)

    def one(step, state):
        source = count - 1 - step
        return combine(state, lax.dynamic_index_in_dim(gathered, source, 0, False))

    return lax.fori_loop(0, ahead, one, state)


def add_decay(earlier, later_part):
    return earlier + later_part


def local(prompt, forget_weight, value_weight, leak, query, next_input, read_gain):
    seqs, span, width = prompt.shape
    heads_here = forget_weight.shape[1] // DK
    flat_rows = prompt.reshape(seqs * span, width)
    gate_pre = jnp.dot(flat_rows, forget_weight, preferred_element_type=jnp.float32).reshape(
        seqs, span, heads_here, DK
    )
    values = jnp.dot(flat_rows, value_weight, preferred_element_type=jnp.float32).astype(
        jnp.bfloat16
    )
    values = values.reshape(seqs, span, heads_here, DV)
    leak_heads = leak.reshape(heads_here, DK)
    inflow = leak_heads * jax.nn.sigmoid(-gate_pre)
    seg_cum = jnp.cumsum(jnp.log1p(-inflow), axis=1)
    seg_total = seg_cum[:, -1]
    weighted = (inflow * jnp.exp(seg_total[:, None] - seg_cum)).astype(jnp.bfloat16)
    seg_state = jnp.einsum("sphk,sphv->shkv", weighted, values, preferred_element_type=jnp.float32)
    next_pre = jnp.dot(next_input, forget_weight, preferred_element_type=jnp.float32).reshape(
        seqs, heads_here, DK
    )
    next_values = jnp.dot(next_input, value_weight, preferred_element_type=jnp.float32).astype(
        jnp.bfloat16
    )
    next_values = next_values.astype(jnp.float32).reshape(seqs, heads_here, DV)
    next_inflow = leak_heads * jax.nn.sigmoid(-next_pre)
    next_forget = 1.0 - next_inflow
    queries = query.astype(jnp.float32).reshape(seqs, heads_here, DK)
    rows_here = DK // lax.axis_size("sp")
    start = lax.axis_index("sp") * rows_here
    later = prefix(seg_total, "sp", add_decay, jnp.zeros_like(seg_total))
    term = jnp.exp(later)[..., None] * seg_state
    owned = lax.psum_scatter(term, "sp", scatter_dimension=2, tiled=True)
    forget_rows = lax.dynamic_slice_in_dim(next_forget, start, rows_here, 2)
    inflow_rows = lax.dynamic_slice_in_dim(next_inflow, start, rows_here, 2)
    query_rows = lax.dynamic_slice_in_dim(queries, start, rows_here, 2)
    read_rows = forget_rows[..., None] * owned + inflow_rows[..., None] * next_values[:, :, None, :]
    partial_read = jnp.sum(query_rows[..., None] * read_rows, axis=2)
    raw_read = lax.psum(partial_read, "sp")
    cache = owned.astype(jnp.bfloat16)
    scaled = raw_read * lax.rsqrt(jnp.mean(raw_read * raw_read, axis=-1, keepdims=True) + 1e-06)
    read_out = (
        (scaled * read_gain.reshape(heads_here, DV))
        .astype(jnp.bfloat16)
        .reshape(seqs, heads_here * DV)
    )
    return (cache, read_out)


def solution(mesh):
    placed = (
        P("gr", "sp", None),
        P(None, "tp"),
        P(None, "tp"),
        P("tp"),
        P("gr", "tp"),
        P("gr", None),
        P("tp"),
    )
    return jax.shard_map(
        fused if mesh.shape["sp"] == 4 else local,
        mesh=mesh,
        in_specs=placed,
        out_specs=(P("gr", "tp", "sp", None), P("gr", "tp")),
        check_vma=False,
    )
```

```python
import functools

import jax
import jax.numpy as jnp
from jax import lax
from jax.experimental import pallas as pl
from jax.experimental.pallas import tpu as pltpu
from jax.sharding import PartitionSpec as P

DK = 128
DV = 128
PAIR = 2
PAD = 16
LAG = 4
F32 = jnp.float32
BF16 = jnp.bfloat16


def suffix_product(x):
    rows = x.shape[0]
    step = 1
    while step < rows:
        x = x * jnp.concatenate([x[step:], jnp.ones((step, x.shape[1]), F32)], axis=0)
        step *= 2
    return x


def kernel(
    seqs, span, chunks,
    prompt, forget_w, value_w, leak, query, nxt, gain,
    cache, read_out,
    x_v, fw_v, vw_v, pad_v, gate_v, val_v, keys_v, qf_v, qi_v, nv_v,
    totals, states, stage1, stage2, reads,
    load_sem, tot_s, tot_r, s1_s, s1_r, s2_s, s2_r, rd_s, rd_r,
):
    me = lax.axis_index("sp")
    count = 4
    xbit, ybit = me % 2, me // 2
    xpeer = me + 1 - 2 * xbit
    ypeer = me + 2 - 4 * ybit
    dpeer = 3 - me
    peers = (xpeer, ypeer, dpeer)
    rows = seqs * span
    wide = PAIR * DK
    kdev = DK // count

    def cols(c):
        return pl.ds(pl.multiple_of(c * wide, wide), wide)

    def load_w(c, which):
        src, dst = ((forget_w, fw_v), (value_w, vw_v))[which]
        return pltpu.make_async_copy(
            src.at[:, cols(c)], dst.at[:, cols(c)], load_sem.at[1 + 2 * c + which]
        )

    load_x = pltpu.make_async_copy(prompt, x_v.at[pl.ds(0, rows)], load_sem.at[0])
    load_x.start()
    load_w(0, 0).start()
    for c in range(chunks):
        if c + 1 < chunks:
            load_w(c + 1, 0).start()
        load_w(c, 1).start()

    barrier = pltpu.get_barrier_semaphore()
    for peer in peers:
        pl.semaphore_signal(barrier, inc=1, device_id={"sp": peer})
    pad_v[...] = jnp.zeros_like(pad_v)
    pad_v[0:seqs, :] = nxt[...].astype(F32)
    x_v[rows:, :] = pad_v[...].astype(BF16)
    pl.semaphore_wait(barrier, 3)

    def tot_copy(c, i):
        return pltpu.make_async_remote_copy(
            src_ref=totals.at[c, me], dst_ref=totals.at[c, me],
            send_sem=tot_s.at[c, i], recv_sem=tot_r.at[c, i],
            device_id={"sp": peers[i]},
        )

    def read_copy(c, i):
        return pltpu.make_async_remote_copy(
            src_ref=reads.at[c, me], dst_ref=reads.at[c, me],
            send_sem=rd_s.at[c, i], recv_sem=rd_r.at[c, i],
            device_id={"sp": peers[i]},
        )

    def s1_copy(c, j):
        bit, peer = ((xbit, xpeer), (ybit, ypeer))[j]
        return pltpu.make_async_remote_copy(
            src_ref=states.at[c, j, 1 - bit], dst_ref=stage1.at[c, j],
            send_sem=s1_s.at[c, j], recv_sem=s1_r.at[c, j],
            device_id={"sp": peer},
        )

    def s2_copy(c, j):
        bit, (bit2, peer) = ((xbit, (ybit, ypeer)), (ybit, (xbit, xpeer)))[j]
        return pltpu.make_async_remote_copy(
            src_ref=states.at[c, j, bit, 1 - bit2], dst_ref=stage2.at[c, j],
            send_sem=s2_s.at[c, j], recv_sem=s2_r.at[c, j],
            device_id={"sp": peer},
        )

    def gates(c):
        load_w(c, 0).wait()
        gate_v[...] = jnp.dot(x_v[...], fw_v[:, cols(c)], preferred_element_type=F32)
        lk = leak[:, cols(c)]
        for s in range(seqs):
            at = slice(s * span, (s + 1) * span)
            inflow = lk * jax.nn.sigmoid(-gate_v[at, :])
            forget = 1.0 - inflow
            after = suffix_product(
                jnp.concatenate([forget[1:], jnp.ones((1, wide), F32)], axis=0)
            )
            keys_v[c % 2, at, :] = inflow * after
            total = forget[0:1] * after[0:1]
            for j in range(PAIR):
                totals[c, me, j * seqs + s : j * seqs + s + 1, :] = total[:, j * DK : (j + 1) * DK]
        n_in = lk * jax.nn.sigmoid(-gate_v[rows : rows + seqs, :])
        q = query[:, cols(c)].astype(F32)
        qf_v[:, cols(c)] = q * (1.0 - n_in)
        qi_v[:, cols(c)] = q * n_in
        for i in range(3):
            tot_copy(c, i).start()

    def segment_states(c):
        load_w(c, 1).wait()
        val_v[...] = jnp.dot(x_v[...], vw_v[:, cols(c)], preferred_element_type=F32).astype(BF16)
        nv_v[:, cols(c)] = val_v[rows:, :].astype(F32)
        for i in range(3):
            tot_copy(c, i).wait_recv()
        later = jnp.ones((PAIR * seqs, DK), F32)
        for source in range(1, count):
            part = totals[c, source]
            later = later * jnp.where(source > me, part, jnp.ones_like(part))
        for j in range(PAIR):
            head = slice(j * DK, (j + 1) * DK)
            for s in range(seqs):
                at = slice(s * span, (s + 1) * span)
                row = j * seqs + s
                weighted = (keys_v[c % 2, at, head] * later[row : row + 1]).astype(BF16)
                keys_v[c % 2, at, head] = weighted.astype(F32)
                state = lax.dot_general(
                    weighted, val_v[at, head], (((0,), (0,)), ((), ())),
                    preferred_element_type=F32,
                )
                for owner in range(count):
                    first, second = (owner % 2, owner // 2)[:: 1 if j == 0 else -1]
                    states[c, j, first, second, s * kdev : (s + 1) * kdev, :] = state[
                        owner * kdev : (owner + 1) * kdev
                    ]
            s1_copy(c, j).start()
        for s in range(seqs):
            at = slice(s * span, (s + 1) * span)
            weighed = keys_v[c % 2, at, :] * qf_v[s : s + 1, cols(c)]
            for j in range(PAIR):
                head = slice(j * DK, (j + 1) * DK)
                a = jnp.sum(weighed[:, head], axis=1, keepdims=True)
                reads[c, me, j * seqs + s : j * seqs + s + 1, :] = jnp.sum(
                    a * val_v[at, head].astype(F32), axis=0, keepdims=True
                )
        for i in range(3):
            read_copy(c, i).start()

    def combine(c):
        for j in range(PAIR):
            bit = (xbit, ybit)[j]
            s1_copy(c, j).wait_recv()
            states[c, j, bit] = states[c, j, bit] + stage1[c, j]
            s2_copy(c, j).start()

    def finish(c):
        for j in range(PAIR):
            bit, bit2 = ((xbit, ybit), (ybit, xbit))[j]
            s2_copy(c, j).wait_recv()
            owned = states[c, j, bit, bit2] + stage2[c, j]
            for s in range(seqs):
                cache[s, c * PAIR + j] = owned[s * kdev : (s + 1) * kdev].astype(BF16)

    load_x.wait()

    def stage(i, carry):
        @pl.when(i < chunks)
        def _():
            gates(i)

        @pl.when(i >= 1)
        def _():
            segment_states(i - 1)

        @pl.when(i >= LAG)
        def _():
            combine(i - LAG)

        return carry

    lax.fori_loop(0, chunks + 1, stage, 0)
    for c in range(chunks + 1 - LAG, chunks):
        combine(c)
    for c in range(chunks - 1):
        finish(c)
    for c in range(chunks):
        for i in range(3):
            read_copy(c, i).wait_recv()
        raw = reads[c, 0]
        for source in range(1, count):
            raw = raw + reads[c, source]
        for j in range(PAIR):
            head = slice((c * PAIR + j) * DV, (c * PAIR + j + 1) * DV)
            inner = jnp.sum(qi_v[:, head], axis=1, keepdims=True)
            r = raw[j * seqs : (j + 1) * seqs] + inner * nv_v[0:seqs, head]
            scale = lax.rsqrt(jnp.mean(r * r, axis=1, keepdims=True) + 1e-06)
            read_out[:, head] = (r * scale * gain[:, head]).astype(BF16)
    finish(chunks - 1)
    for c in range(chunks):
        for i in range(3):
            tot_copy(c, i).wait_send()
        for j in range(PAIR):
            s1_copy(c, j).wait_send()
            s2_copy(c, j).wait_send()
        for i in range(3):
            read_copy(c, i).wait_send()


def hand_over(cache_in, read_in, cache, read_out):
    cache[...] = cache_in[...]
    read_out[...] = read_in[...]


def fused(prompt, forget_weight, value_weight, leak, query, next_input, read_gain):
    seqs, span, width = prompt.shape
    here = forget_weight.shape[1]
    heads = here // DK
    chunks = heads // PAIR
    wide = PAIR * DK
    count = lax.axis_size("sp")
    kdev = DK // count
    rows = seqs * span
    anyspace = pl.BlockSpec(memory_space=pl.ANY)
    vm = pl.BlockSpec(memory_space=pltpu.VMEM)
    dma = pltpu.SemaphoreType.DMA
    made = pl.pallas_call(
        functools.partial(kernel, seqs, span, chunks),
        out_shape=(
            jax.ShapeDtypeStruct((seqs, heads, kdev, DV), BF16),
            jax.ShapeDtypeStruct((seqs, here), BF16),
        ),
        in_specs=[anyspace, anyspace, anyspace, vm, vm, vm, vm],
        out_specs=(vm, vm),
        scratch_shapes=[
            pltpu.VMEM((rows + PAD, width), BF16),
            pltpu.VMEM((width, here), BF16),
            pltpu.VMEM((width, here), BF16),
            pltpu.VMEM((PAD, width), F32),
            pltpu.VMEM((rows + PAD, wide), F32),
            pltpu.VMEM((rows + PAD, wide), BF16),
            pltpu.VMEM((2, rows, wide), F32),
            pltpu.VMEM((seqs, here), F32),
            pltpu.VMEM((seqs, here), F32),
            pltpu.VMEM((PAD, here), F32),
            pltpu.VMEM((chunks, count, PAIR * seqs, DK), F32),
            pltpu.VMEM((chunks, PAIR, 2, 2, seqs * kdev, DV), F32),
            pltpu.VMEM((chunks, PAIR, 2, seqs * kdev, DV), F32),
            pltpu.VMEM((chunks, PAIR, seqs * kdev, DV), F32),
            pltpu.VMEM((chunks, count, PAIR * seqs, DV), F32),
            dma((1 + 2 * chunks,)),
            dma((chunks, 3)),
            dma((chunks, 3)),
            dma((chunks, PAIR)),
            dma((chunks, PAIR)),
            dma((chunks, PAIR)),
            dma((chunks, PAIR)),
            dma((chunks, 3)),
            dma((chunks, 3)),
        ],
        compiler_params=pltpu.CompilerParams(
            collective_id=0, has_side_effects=True, vmem_limit_bytes=60 * 1024 * 1024
        ),
    )(
        prompt.reshape(rows, width), forget_weight, value_weight, leak.reshape(1, here),
        query, next_input, read_gain.reshape(1, here),
    )
    return pl.pallas_call(
        hand_over,
        out_shape=tuple(jax.ShapeDtypeStruct(a.shape, a.dtype) for a in made),
        in_specs=[vm, vm],
        out_specs=(vm, vm),
    )(*made)


def prefix(part, axis, combine, identity):
    count = lax.axis_size(axis)
    place = lax.axis_index(axis)
    ahead = count - 1 - place
    gathered = lax.all_gather(part, axis)
    state = jnp.zeros_like(part) + jnp.asarray(identity, part.dtype)

    def one(step, state):
        source = count - 1 - step
        return combine(state, lax.dynamic_index_in_dim(gathered, source, 0, False))

    return lax.fori_loop(0, ahead, one, state)


def add_decay(earlier, later_part):
    return earlier + later_part


def local(prompt, forget_weight, value_weight, leak, query, next_input, read_gain):
    seqs, span, width = prompt.shape
    heads_here = forget_weight.shape[1] // DK
    flat_rows = prompt.reshape(seqs * span, width)
    gate_pre = jnp.dot(flat_rows, forget_weight, preferred_element_type=jnp.float32).reshape(
        seqs, span, heads_here, DK
    )
    values = jnp.dot(flat_rows, value_weight, preferred_element_type=jnp.float32).astype(
        jnp.bfloat16
    )
    values = values.reshape(seqs, span, heads_here, DV)
    leak_heads = leak.reshape(heads_here, DK)
    inflow = leak_heads * jax.nn.sigmoid(-gate_pre)
    seg_cum = jnp.cumsum(jnp.log1p(-inflow), axis=1)
    seg_total = seg_cum[:, -1]
    weighted = (inflow * jnp.exp(seg_total[:, None] - seg_cum)).astype(jnp.bfloat16)
    seg_state = jnp.einsum("sphk,sphv->shkv", weighted, values, preferred_element_type=jnp.float32)
    next_pre = jnp.dot(next_input, forget_weight, preferred_element_type=jnp.float32).reshape(
        seqs, heads_here, DK
    )
    next_values = jnp.dot(next_input, value_weight, preferred_element_type=jnp.float32).astype(
        jnp.bfloat16
    )
    next_values = next_values.astype(jnp.float32).reshape(seqs, heads_here, DV)
    next_inflow = leak_heads * jax.nn.sigmoid(-next_pre)
    next_forget = 1.0 - next_inflow
    queries = query.astype(jnp.float32).reshape(seqs, heads_here, DK)
    rows_here = DK // lax.axis_size("sp")
    start = lax.axis_index("sp") * rows_here
    later = prefix(seg_total, "sp", add_decay, jnp.zeros_like(seg_total))
    term = jnp.exp(later)[..., None] * seg_state
    owned = lax.psum_scatter(term, "sp", scatter_dimension=2, tiled=True)
    forget_rows = lax.dynamic_slice_in_dim(next_forget, start, rows_here, 2)
    inflow_rows = lax.dynamic_slice_in_dim(next_inflow, start, rows_here, 2)
    query_rows = lax.dynamic_slice_in_dim(queries, start, rows_here, 2)
    read_rows = forget_rows[..., None] * owned + inflow_rows[..., None] * next_values[:, :, None, :]
    partial_read = jnp.sum(query_rows[..., None] * read_rows, axis=2)
    raw_read = lax.psum(partial_read, "sp")
    cache = owned.astype(jnp.bfloat16)
    scaled = raw_read * lax.rsqrt(jnp.mean(raw_read * raw_read, axis=-1, keepdims=True) + 1e-06)
    read_out = (
        (scaled * read_gain.reshape(heads_here, DV))
        .astype(jnp.bfloat16)
        .reshape(seqs, heads_here * DV)
    )
    return (cache, read_out)


def solution(mesh):
    placed = (
        P("gr", "sp", None),
        P(None, "tp"),
        P(None, "tp"),
        P("tp"),
        P("gr", "tp"),
        P("gr", None),
        P("tp"),
    )
    return jax.shard_map(
        fused if mesh.shape["sp"] == 4 else local,
        mesh=mesh,
        in_specs=placed,
        out_specs=(P("gr", "tp", "sp", None), P("gr", "tp")),
        check_vma=False,
    )
```

```python
import functools

import jax
import jax.numpy as jnp
from jax import lax
from jax.experimental import pallas as pl
from jax.experimental.pallas import tpu as pltpu
from jax.sharding import PartitionSpec as P

DK = 128
DV = 128
PAIR = 2
PAD = 16
LAG = 4
F32 = jnp.float32
BF16 = jnp.bfloat16


def suffix_product(x):
    rows = x.shape[0]
    step = 1
    while step < rows:
        x = x * jnp.concatenate([x[step:], jnp.ones((step, x.shape[1]), F32)], axis=0)
        step *= 2
    return x


def kernel(
    seqs, span, chunks,
    prompt, forget_w, value_w, leak, query, nxt, gain,
    cache, read_out,
    x_v, fw_v, vw_v, pad_v, gate_v, val_v, keys_v, qf_v, qi_v, nv_v,
    totals, states, stage1, stage2, reads,
    load_sem, tot_s, tot_r, s1_s, s1_r, s2_s, s2_r, rd_s, rd_r,
):
    me = lax.axis_index("sp")
    count = 4
    xbit, ybit = me % 2, me // 2
    xpeer = me + 1 - 2 * xbit
    ypeer = me + 2 - 4 * ybit
    dpeer = 3 - me
    peers = (xpeer, ypeer, dpeer)
    rows = seqs * span
    wide = PAIR * DK
    kdev = DK // count

    def cols(c):
        return pl.ds(pl.multiple_of(c * wide, wide), wide)

    def load_w(c, which):
        src, dst = ((forget_w, fw_v), (value_w, vw_v))[which]
        return pltpu.make_async_copy(
            src.at[:, cols(c)], dst.at[:, cols(c)], load_sem.at[1 + 2 * c + which]
        )

    load_x = pltpu.make_async_copy(prompt, x_v.at[pl.ds(0, rows)], load_sem.at[0])
    load_x.start()
    load_w(0, 0).start()
    for c in range(chunks):
        if c + 1 < chunks:
            load_w(c + 1, 0).start()
        load_w(c, 1).start()

    barrier = pltpu.get_barrier_semaphore()
    for peer in peers:
        pl.semaphore_signal(barrier, inc=1, device_id={"sp": peer})
    pad_v[...] = jnp.zeros_like(pad_v)
    pad_v[0:seqs, :] = nxt[...].astype(F32)
    x_v[rows:, :] = pad_v[...].astype(BF16)
    pl.semaphore_wait(barrier, 3)

    def tot_copy(c, i):
        return pltpu.make_async_remote_copy(
            src_ref=totals.at[c, me], dst_ref=totals.at[c, me],
            send_sem=tot_s.at[c, i], recv_sem=tot_r.at[c, i],
            device_id={"sp": peers[i]},
        )

    def read_copy(c, i):
        return pltpu.make_async_remote_copy(
            src_ref=reads.at[c, me], dst_ref=reads.at[c, me],
            send_sem=rd_s.at[c, i], recv_sem=rd_r.at[c, i],
            device_id={"sp": peers[i]},
        )

    def s1_copy(c, j):
        bit, peer = ((xbit, xpeer), (ybit, ypeer))[j]
        return pltpu.make_async_remote_copy(
            src_ref=states.at[c, j, 1 - bit], dst_ref=stage1.at[c, j],
            send_sem=s1_s.at[c, j], recv_sem=s1_r.at[c, j],
            device_id={"sp": peer},
        )

    def s2_copy(c, j):
        bit, (bit2, peer) = ((xbit, (ybit, ypeer)), (ybit, (xbit, xpeer)))[j]
        return pltpu.make_async_remote_copy(
            src_ref=states.at[c, j, bit, 1 - bit2], dst_ref=stage2.at[c, j],
            send_sem=s2_s.at[c, j], recv_sem=s2_r.at[c, j],
            device_id={"sp": peer},
        )

    def gates(c):
        load_w(c, 0).wait()
        gate_v[...] = jnp.dot(x_v[...], fw_v[:, cols(c)], preferred_element_type=F32)
        lk = leak[:, cols(c)]
        for s in range(seqs):
            at = slice(s * span, (s + 1) * span)
            inflow = lk * jax.nn.sigmoid(-gate_v[at, :])
            forget = 1.0 - inflow
            after = suffix_product(
                jnp.concatenate([forget[1:], jnp.ones((1, wide), F32)], axis=0)
            )
            keys_v[c % 2, at, :] = inflow * after
            total = forget[0:1] * after[0:1]
            for j in range(PAIR):
                totals[c, me, j * seqs + s : j * seqs + s + 1, :] = total[:, j * DK : (j + 1) * DK]
        n_in = lk * jax.nn.sigmoid(-gate_v[rows : rows + seqs, :])
        q = query[:, cols(c)].astype(F32)
        qf_v[:, cols(c)] = q * (1.0 - n_in)
        qi_v[:, cols(c)] = q * n_in
        for i in range(3):
            tot_copy(c, i).start()

    def segment_states(c):
        load_w(c, 1).wait()
        val_v[...] = jnp.dot(x_v[...], vw_v[:, cols(c)], preferred_element_type=F32).astype(BF16)
        nv_v[:, cols(c)] = val_v[rows:, :].astype(F32)
        for i in range(3):
            tot_copy(c, i).wait_recv()
        later = jnp.ones((PAIR * seqs, DK), F32)
        for source in range(1, count):
            part = totals[c, source]
            later = later * jnp.where(source > me, part, jnp.ones_like(part))
        for s in range(seqs):
            at = slice(s * span, (s + 1) * span)
            to_end = jnp.concatenate(
                [later[j * seqs + s : j * seqs + s + 1] for j in range(PAIR)], axis=1
            )
            weighted = (keys_v[c % 2, at, :] * to_end).astype(BF16)
            weighed = weighted.astype(F32) * qf_v[s : s + 1, cols(c)]
            for j in range(PAIR):
                head = slice(j * DK, (j + 1) * DK)
                v = val_v[at, head]
                state = lax.dot_general(
                    weighted[:, head], v, (((0,), (0,)), ((), ())),
                    preferred_element_type=F32,
                )
                for owner in range(count):
                    first, second = (owner % 2, owner // 2)[:: 1 if j == 0 else -1]
                    states[c, j, first, second, s * kdev : (s + 1) * kdev, :] = state[
                        owner * kdev : (owner + 1) * kdev
                    ]
                a = jnp.sum(weighed[:, head], axis=1, keepdims=True)
                reads[c, me, j * seqs + s : j * seqs + s + 1, :] = jnp.sum(
                    a * v.astype(F32), axis=0, keepdims=True
                )
        for j in range(PAIR):
            s1_copy(c, j).start()
        for i in range(3):
            read_copy(c, i).start()

    def combine(c):
        for j in range(PAIR):
            bit = (xbit, ybit)[j]
            s1_copy(c, j).wait_recv()
            states[c, j, bit] = states[c, j, bit] + stage1[c, j]
            s2_copy(c, j).start()

    def finish(c):
        for j in range(PAIR):
            bit, bit2 = ((xbit, ybit), (ybit, xbit))[j]
            s2_copy(c, j).wait_recv()
            owned = states[c, j, bit, bit2] + stage2[c, j]
            for s in range(seqs):
                cache[s, c * PAIR + j] = owned[s * kdev : (s + 1) * kdev].astype(BF16)

    load_x.wait()

    def stage(i, carry):
        @pl.when(i < chunks)
        def _():
            gates(i)

        @pl.when(i >= 1)
        def _():
            segment_states(i - 1)

        @pl.when(i >= LAG)
        def _():
            combine(i - LAG)

        return carry

    lax.fori_loop(0, chunks + 1, stage, 0)
    for c in range(chunks + 1 - LAG, chunks):
        combine(c)
    for c in range(chunks - 1):
        finish(c)
    for c in range(chunks):
        for i in range(3):
            read_copy(c, i).wait_recv()
        raw = reads[c, 0]
        for source in range(1, count):
            raw = raw + reads[c, source]
        for j in range(PAIR):
            head = slice((c * PAIR + j) * DV, (c * PAIR + j + 1) * DV)
            inner = jnp.sum(qi_v[:, head], axis=1, keepdims=True)
            r = raw[j * seqs : (j + 1) * seqs] + inner * nv_v[0:seqs, head]
            scale = lax.rsqrt(jnp.mean(r * r, axis=1, keepdims=True) + 1e-06)
            read_out[:, head] = (r * scale * gain[:, head]).astype(BF16)
    finish(chunks - 1)
    for c in range(chunks):
        for i in range(3):
            tot_copy(c, i).wait_send()
        for j in range(PAIR):
            s1_copy(c, j).wait_send()
            s2_copy(c, j).wait_send()
        for i in range(3):
            read_copy(c, i).wait_send()


def hand_over(cache_in, read_in, cache, read_out):
    cache[...] = cache_in[...]
    read_out[...] = read_in[...]


def fused(prompt, forget_weight, value_weight, leak, query, next_input, read_gain):
    seqs, span, width = prompt.shape
    here = forget_weight.shape[1]
    heads = here // DK
    chunks = heads // PAIR
    wide = PAIR * DK
    count = lax.axis_size("sp")
    kdev = DK // count
    rows = seqs * span
    anyspace = pl.BlockSpec(memory_space=pl.ANY)
    vm = pl.BlockSpec(memory_space=pltpu.VMEM)
    dma = pltpu.SemaphoreType.DMA
    made = pl.pallas_call(
        functools.partial(kernel, seqs, span, chunks),
        out_shape=(
            jax.ShapeDtypeStruct((seqs, heads, kdev, DV), BF16),
            jax.ShapeDtypeStruct((seqs, here), BF16),
        ),
        in_specs=[anyspace, anyspace, anyspace, vm, vm, vm, vm],
        out_specs=(vm, vm),
        scratch_shapes=[
            pltpu.VMEM((rows + PAD, width), BF16),
            pltpu.VMEM((width, here), BF16),
            pltpu.VMEM((width, here), BF16),
            pltpu.VMEM((PAD, width), F32),
            pltpu.VMEM((rows + PAD, wide), F32),
            pltpu.VMEM((rows + PAD, wide), BF16),
            pltpu.VMEM((2, rows, wide), F32),
            pltpu.VMEM((seqs, here), F32),
            pltpu.VMEM((seqs, here), F32),
            pltpu.VMEM((PAD, here), F32),
            pltpu.VMEM((chunks, count, PAIR * seqs, DK), F32),
            pltpu.VMEM((chunks, PAIR, 2, 2, seqs * kdev, DV), F32),
            pltpu.VMEM((chunks, PAIR, 2, seqs * kdev, DV), F32),
            pltpu.VMEM((chunks, PAIR, seqs * kdev, DV), F32),
            pltpu.VMEM((chunks, count, PAIR * seqs, DV), F32),
            dma((1 + 2 * chunks,)),
            dma((chunks, 3)),
            dma((chunks, 3)),
            dma((chunks, PAIR)),
            dma((chunks, PAIR)),
            dma((chunks, PAIR)),
            dma((chunks, PAIR)),
            dma((chunks, 3)),
            dma((chunks, 3)),
        ],
        compiler_params=pltpu.CompilerParams(
            collective_id=0, has_side_effects=True, vmem_limit_bytes=60 * 1024 * 1024
        ),
    )(
        prompt.reshape(rows, width), forget_weight, value_weight, leak.reshape(1, here),
        query, next_input, read_gain.reshape(1, here),
    )
    return pl.pallas_call(
        hand_over,
        out_shape=tuple(jax.ShapeDtypeStruct(a.shape, a.dtype) for a in made),
        in_specs=[vm, vm],
        out_specs=(vm, vm),
    )(*made)


def prefix(part, axis, combine, identity):
    count = lax.axis_size(axis)
    place = lax.axis_index(axis)
    ahead = count - 1 - place
    gathered = lax.all_gather(part, axis)
    state = jnp.zeros_like(part) + jnp.asarray(identity, part.dtype)

    def one(step, state):
        source = count - 1 - step
        return combine(state, lax.dynamic_index_in_dim(gathered, source, 0, False))

    return lax.fori_loop(0, ahead, one, state)


def add_decay(earlier, later_part):
    return earlier + later_part


def local(prompt, forget_weight, value_weight, leak, query, next_input, read_gain):
    seqs, span, width = prompt.shape
    heads_here = forget_weight.shape[1] // DK
    flat_rows = prompt.reshape(seqs * span, width)
    gate_pre = jnp.dot(flat_rows, forget_weight, preferred_element_type=jnp.float32).reshape(
        seqs, span, heads_here, DK
    )
    values = jnp.dot(flat_rows, value_weight, preferred_element_type=jnp.float32).astype(
        jnp.bfloat16
    )
    values = values.reshape(seqs, span, heads_here, DV)
    leak_heads = leak.reshape(heads_here, DK)
    inflow = leak_heads * jax.nn.sigmoid(-gate_pre)
    seg_cum = jnp.cumsum(jnp.log1p(-inflow), axis=1)
    seg_total = seg_cum[:, -1]
    weighted = (inflow * jnp.exp(seg_total[:, None] - seg_cum)).astype(jnp.bfloat16)
    seg_state = jnp.einsum("sphk,sphv->shkv", weighted, values, preferred_element_type=jnp.float32)
    next_pre = jnp.dot(next_input, forget_weight, preferred_element_type=jnp.float32).reshape(
        seqs, heads_here, DK
    )
    next_values = jnp.dot(next_input, value_weight, preferred_element_type=jnp.float32).astype(
        jnp.bfloat16
    )
    next_values = next_values.astype(jnp.float32).reshape(seqs, heads_here, DV)
    next_inflow = leak_heads * jax.nn.sigmoid(-next_pre)
    next_forget = 1.0 - next_inflow
    queries = query.astype(jnp.float32).reshape(seqs, heads_here, DK)
    rows_here = DK // lax.axis_size("sp")
    start = lax.axis_index("sp") * rows_here
    later = prefix(seg_total, "sp", add_decay, jnp.zeros_like(seg_total))
    term = jnp.exp(later)[..., None] * seg_state
    owned = lax.psum_scatter(term, "sp", scatter_dimension=2, tiled=True)
    forget_rows = lax.dynamic_slice_in_dim(next_forget, start, rows_here, 2)
    inflow_rows = lax.dynamic_slice_in_dim(next_inflow, start, rows_here, 2)
    query_rows = lax.dynamic_slice_in_dim(queries, start, rows_here, 2)
    read_rows = forget_rows[..., None] * owned + inflow_rows[..., None] * next_values[:, :, None, :]
    partial_read = jnp.sum(query_rows[..., None] * read_rows, axis=2)
    raw_read = lax.psum(partial_read, "sp")
    cache = owned.astype(jnp.bfloat16)
    scaled = raw_read * lax.rsqrt(jnp.mean(raw_read * raw_read, axis=-1, keepdims=True) + 1e-06)
    read_out = (
        (scaled * read_gain.reshape(heads_here, DV))
        .astype(jnp.bfloat16)
        .reshape(seqs, heads_here * DV)
    )
    return (cache, read_out)


def solution(mesh):
    placed = (
        P("gr", "sp", None),
        P(None, "tp"),
        P(None, "tp"),
        P("tp"),
        P("gr", "tp"),
        P("gr", None),
        P("tp"),
    )
    return jax.shard_map(
        fused if mesh.shape["sp"] == 4 else local,
        mesh=mesh,
        in_specs=placed,
        out_specs=(P("gr", "tp", "sp", None), P("gr", "tp")),
        check_vma=False,
    )
```
